512 devices in a mesh: ep: 32 (over z, x), tp: 16 (over y, core).
Axes of the slice: x: 4, y: 8, z: 8, core: 2. Of those that a mesh axis runs over, the one named last changes fastest.
Arguments:
- mixer_input: bfloat16 [4096, 2048], P('ep'), may hold values from -6 to 6
- mixer_gain: float32 [2048], replicated, may hold values from 0.1 to 1.9
- outer_weight: bfloat16 [2048, 1024], P(None, 'tp'), may hold values from -0.125 to 0.125
- inner_weight: bfloat16 [2048, 1024], P(None, 'tp'), may hold values from -0.125 to 0.125
- value_weight: bfloat16 [2048, 1024], P(None, 'tp'), may hold values from -0.125 to 0.125
- conv_kernel: bfloat16 [3, 1024], P(None, 'tp'), may hold values from -3 to 3
- group_gain: float32 [1024], P('tp'), may hold values from 0.1 to 1.9
- mixer_out_weight: bfloat16 [1024, 2048], P(None, 'tp'), may hold values from -0.1875 to 0.1875
- expert_input: bfloat16 [8192, 2048], P('ep'), may hold values from -6 to 6
- expert_gain: float32 [2048], replicated, may hold values from 0.1 to 1.9
- routes: int32 [8192, 2], P('ep'), may hold values from 0 to 31, all different within a row; in each aligned block of 256 rows (0 to 255, 256 to 511, ...) at most 32 rows name the same one
- route_weight: float32 [8192, 2], P('ep'), may hold values from 0.1 to 1
- expert_gate: bfloat16 [32, 2048, 3584], P('ep', None, 'tp'), may hold values from -0.125 to 0.125
- expert_up: bfloat16 [32, 2048, 3584], P('ep', None, 'tp'), may hold values from -0.125 to 0.125
- expert_down: bfloat16 [32, 3584, 2048], P('ep', None, 'tp'), may hold values from -0.09375 to 0.09375
Outputs:
- mixed_tokens: bfloat16 [4096, 2048], P('ep', 'tp')
- expert_tokens: bfloat16 [8192, 2048], P('ep', 'tp')
The draws below stay inside these ranges and needn't reach their ends.
Inputs may be any that keep to these rules, and one draw needn't show every extreme that they name: `routes`: each row names 2 different experts. Within the rows of one index of ep no expert is named by more than 32 rows, a bound that some block reaches of them.
All inputs are finite; a program needn't handle non-finite values.
Results may differ from the reference program's by a relative error of at most 0.014.
Values may be sent and summed in bfloat16 or wider, within the bound.
A program may use at most 64 MiB of HBM per device.

```python
import math
import jax
import jax.numpy as jnp
import numpy as np
from jax import lax

D = 2048
CONV = 1024
GROUP = 64
FF = 3584
TOP = 2
EXP_ROWS = 256
EXPERTS = 32
CAP = 32
MIX_TOKENS = 4096
EXP_TOKENS = 8192
N_EP = 32


def level_of(rng, extent, cuts, smallest, high):
    loudness = 1.0
    for dim, blocks in cuts:
        draws = jax.random.uniform(jax.random.fold_in(jax.random.fold_in(rng, 6), dim), (blocks,), jnp.float32, smallest / len(cuts), high / len(cuts))
        loudness = loudness * jnp.repeat(jnp.exp(draws), extent[dim] // blocks).reshape((-1,) + (1,) * (len(extent) - 1 - dim))
    return loudness


def assign_block(own_key, own, number, rows, count, top, bound, skew):
    ranking = jax.random.permutation(own_key, count)
    packed, common = load_shares(count, rows * top, bound, skew, True), load_shares(count, rows * top, bound, skew, False)
    places = jnp.arange(count)

    def named(tallies, turn):
        used = int((tallies > 0).sum())
        fixed = max(1, used // 4)
        passed = fixed + (places - fixed + turn * (used - fixed)) % max(1, count - fixed)
        return jnp.zeros((count,), jnp.int32).at[ranking[jnp.where(places < fixed, places, passed)]].set(jnp.asarray(tallies, jnp.int32))

    tallies = jnp.where(number % 4 == 0, named(packed, number // 4), named(common, number - number // 4 - 1))
    mixed = jax.random.permutation(jax.random.fold_in(own, 3), count)
    source_of, taker = mixed[0:count // 2 * 2:2], mixed[1:count // 2 * 2:2]
    room = jnp.minimum(tallies[source_of] - 1, bound - tallies[taker]) // 2
    room = jnp.where((source_of == ranking[0]) | (taker == ranking[0]) | (tallies[taker] == 0), 0, jnp.maximum(room, 0))
    passed = jax.random.randint(jax.random.fold_in(own, 4), (count // 2,), 0, 1 << 20) % (room + 1)
    tallies = tallies.at[source_of].add(-passed).at[taker].add(passed)
    members = jnp.searchsorted(jnp.cumsum(tallies), jnp.arange(rows * top), side="right").astype(jnp.int32)
    table = members.reshape(top, rows).T
    table = table[jax.random.permutation(jax.random.fold_in(own, 1), rows)]
    turn = jax.random.randint(jax.random.fold_in(own, 2), (rows, 1), 0, top)
    return jnp.take_along_axis(table, (jnp.arange(top)[None, :] + turn) % top, axis=1)


def load_shares(count, total, most, skew, full):
    loads = [(1 << 20) // math.isqrt(rank ** skew) + 1 for rank in range(1, count + 1)]
    largest = most if full else min(most, max(-(-total // count), total * loads[0] // sum(loads)))
    least = 1 if total - largest >= count - 1 else 0
    holding, surplus = [largest] + [least] * (count - 1), total - largest - least * (count - 1)
    while surplus > 0:
        movable = [i for i in range(1, count) if holding[i] < largest] or [i for i in range(1, count) if holding[i] < most]
        whole, remaining = sum([loads[i] for i in movable]), surplus
        for i in movable:
            addition = min(most - holding[i], max(1, remaining * loads[i] // whole), surplus)
            holding[i] = holding[i] + addition
            surplus = surplus - addition
    return np.array(holding)


def scatter_about(stream_key, dims, spread, limit, shards=(), kind=jnp.bfloat16):
    values = spread * jax.random.normal(stream_key, dims, jnp.float32)
    if shards:
        values = values * level_of(stream_key, dims, shards, -0.22, 0.18)
    return jnp.clip(values, -limit, limit).astype(kind)


def setup_inputs(seed: int = 0) -> dict:
    splits = jax.random.split(jax.random.key(seed), 16)
    mixer_input = scatter_about(splits[0], (MIX_TOKENS, D), 1.0, 6.0, ((0, 32),))
    mixer_gain = jnp.clip(1.0 + 0.18 * jax.random.normal(splits[1], (D,), jnp.float32), 0.1, 1.9)
    outer_weight = scatter_about(splits[2], (D, CONV), D ** -0.5, 0.125, ((1, 16),))
    inner_weight = scatter_about(splits[3], (D, CONV), D ** -0.5, 0.125, ((1, 16),))
    value_weight = scatter_about(splits[4], (D, CONV), D ** -0.5, 0.125, ((1, 16),))
    conv_kernel = scatter_about(splits[5], (3, CONV), 0.6, 3.0, ((1, 16),))
    group_gain = jnp.clip(1.0 + 0.18 * jax.random.normal(splits[6], (CONV,), jnp.float32), 0.1, 1.9)
    mixer_out_weight = scatter_about(splits[7], (CONV, D), CONV ** -0.5, 0.1875, ((1, 16),))
    expert_input = scatter_about(splits[8], (EXP_TOKENS, D), 1.0, 6.0, ((0, 32),))
    expert_gain = jnp.clip(1.0 + 0.18 * jax.random.normal(splits[9], (D,), jnp.float32), 0.1, 1.9)
    routes_keys = jax.random.split(jax.random.fold_in(splits[10], 1), EXP_TOKENS // EXP_ROWS)
    routes_turns = jax.random.permutation(jax.random.fold_in(splits[10], 3), EXP_TOKENS // EXP_ROWS)
    routes = jax.vmap(lambda own, number: assign_block(jax.random.fold_in(splits[10], 2), own, number, EXP_ROWS, EXPERTS, TOP, CAP, 2))(routes_keys, routes_turns).reshape((EXP_TOKENS, TOP))
    route_weight = jnp.clip(0.1 + 0.9 * jax.random.uniform(splits[11], (EXP_TOKENS, TOP), jnp.float32) ** level_of(splits[11], (EXP_TOKENS, TOP), ((0, 32),), -0.2, 0.2), 0.1, 1.0)
    expert_gate = scatter_about(splits[12], (EXPERTS, D, FF), D ** -0.5, 0.125, ((0, 32), (2, 16)))
    expert_up = scatter_about(splits[13], (EXPERTS, D, FF), D ** -0.5, 0.125, ((0, 32), (2, 16)))
    expert_down = scatter_about(splits[14], (EXPERTS, FF, D), FF ** -0.5, 0.09375, ((0, 32), (2, 16)))
    return dict(mixer_input=mixer_input, mixer_gain=mixer_gain, outer_weight=outer_weight, inner_weight=inner_weight, value_weight=value_weight, conv_kernel=conv_kernel, group_gain=group_gain, mixer_out_weight=mixer_out_weight, expert_input=expert_input, expert_gain=expert_gain, routes=routes, route_weight=route_weight, expert_gate=expert_gate, expert_up=expert_up, expert_down=expert_down)


EPS = 1e-06

def rms_scale(values, gain):
    floats = values.astype(jnp.float32)
    scale = lax.rsqrt(lax.optimization_barrier(jnp.mean(floats * floats, axis=-1, keepdims=True)) + EPS)
    return floats * scale * gain.astype(jnp.float32)

def run_expert(operands):
    rows, gate_part, up_part, down_part = operands
    gate = jnp.dot(rows, gate_part, preferred_element_type=jnp.float32)
    up_value = jnp.dot(rows, up_part, preferred_element_type=jnp.float32)
    hidden = (jax.nn.silu(gate) * up_value).astype(jnp.bfloat16)
    return jnp.dot(hidden, down_part, preferred_element_type=jnp.float32).astype(jnp.bfloat16)

def reference(mixer_input, mixer_gain, outer_weight, inner_weight, value_weight, conv_kernel, group_gain, mixer_out_weight, expert_input, expert_gain, routes, route_weight, expert_gate, expert_up, expert_down):
    count = mixer_input.shape[0]
    normed_a = rms_scale(mixer_input, mixer_gain).astype(jnp.bfloat16)
    outer = jnp.dot(normed_a, outer_weight, preferred_element_type=jnp.float32).astype(jnp.bfloat16)
    inner = jnp.dot(normed_a, inner_weight, preferred_element_type=jnp.float32).astype(jnp.bfloat16)
    values = jnp.dot(normed_a, value_weight, preferred_element_type=jnp.float32).astype(jnp.bfloat16)
    product = inner.astype(jnp.float32) * values.astype(jnp.float32)
    padded = jnp.pad(product, ((2, 0), (0, 0)))
    kernel = conv_kernel.astype(jnp.float32)
    conv_sum = kernel[0] * padded[0:count] + kernel[1] * padded[1:count + 1] + kernel[2] * padded[2:count + 2]
    gated = outer.astype(jnp.float32) * conv_sum
    grouped = gated.reshape(count, CONV // GROUP, GROUP)
    grouped = rms_scale(grouped, group_gain.reshape(CONV // GROUP, GROUP))
    grouped = grouped.reshape(count, CONV).astype(jnp.bfloat16)
    mixed_tokens = jnp.dot(grouped, mixer_out_weight, preferred_element_type=jnp.float32).astype(jnp.bfloat16)
    normed_b = rms_scale(expert_input, expert_gain).astype(jnp.bfloat16)
    picks = routes.reshape(N_EP, EXP_ROWS * TOP).astype(jnp.int32)
    onehot = (picks[:, :, None] == jnp.arange(EXPERTS, dtype=jnp.int32)[None, None, :]).astype(jnp.int32)
    earlier = jnp.cumsum(onehot, axis=1) - onehot
    rank = lax.optimization_barrier(jnp.sum(earlier * onehot, axis=2)).astype(jnp.int32)
    slot = (picks * CAP + rank).astype(jnp.int32)
    token = (jnp.arange(EXP_ROWS * TOP, dtype=jnp.int32) // TOP).astype(jnp.int32)
    source = jnp.arange(N_EP, dtype=jnp.int32)[:, None]
    table = jnp.zeros((N_EP, EXPERTS * CAP), jnp.int32).at[source, slot].set(token[None, :] + 1)
    valid = table > 0
    row_index = (source * EXP_ROWS + jnp.maximum(table - 1, 0)).astype(jnp.int32)
    buffer = jnp.where(valid[..., None], jnp.take(normed_b, row_index, axis=0), 0).astype(jnp.bfloat16)
    per_expert = buffer.reshape(N_EP, EXPERTS, CAP, D).transpose(1, 0, 2, 3).reshape(EXPERTS, N_EP * CAP, D)
    outputs = lax.map(run_expert, (per_expert, expert_gate, expert_up, expert_down))
    flat_out = outputs.reshape(EXPERTS * N_EP * CAP, D)
    position = (picks * (N_EP * CAP) + source * CAP + rank).astype(jnp.int32)
    chosen = jnp.take(flat_out, position.reshape(-1), axis=0).astype(jnp.float32).reshape(N_EP * EXP_ROWS, TOP, D)
    weighted = lax.optimization_barrier(jnp.sum(chosen * route_weight.astype(jnp.float32)[..., None], axis=1))
    expert_tokens = weighted.astype(jnp.bfloat16)
    return (mixed_tokens, expert_tokens)
```

```python
import functools

import jax
import jax.numpy as jnp
from jax import lax
from jax.experimental import pallas as pl
from jax.experimental.pallas import tpu as pltpu
from jax.sharding import PartitionSpec as P

EPS = 1e-06
MESH = pl.DeviceIdType.MESH
F32 = jnp.float32
BF16 = jnp.bfloat16
NZ, NX = 8, 4
N_EP = NZ * NX
N_Y = 8
N_TP = 2 * N_Y
BATCHES = 4
CAP = 32
PER = N_EP // BATCHES


def hops(n, d):
    return min(d, n - d)


def offset_order():
    pairs = [(dz, dx) for dz in range(NZ) for dx in range(NX)]
    return sorted(pairs, key=lambda o: (hops(NZ, o[0]) + hops(NX, o[1]), hops(NZ, o[0]), o))


OFFSETS = offset_order()
GROUPS = [OFFSETS[8:16], OFFSETS[16:24], OFFSETS[24:32], OFFSETS[0:8]]


def nt(a, b):
    return lax.dot_general(a, b, (((1,), (1,)), ((), ())), preferred_element_type=F32)


def nn(a, b):
    return lax.dot_general(a, b, (((1,), (0,)), ((), ())), preferred_element_type=F32)


def eye(n):
    return (
        lax.broadcasted_iota(jnp.int32, (n, n), 0) == lax.broadcasted_iota(jnp.int32, (n, n), 1)
    )


def column(row, mask):
    return jnp.sum(jnp.where(mask, row, 0.0), axis=1, keepdims=True)


def kernel(
    mixin_h, mgain_h, outer_h, inner_h, value_h, conv_h, ggain_h, mout_h,
    expin_h, egain_h, routes_h, rweight_h, gate_h, up_h, down_h,
    mixed_o, tokens_o,
    mixin, mgain, mproj, conv, ggain, mout,
    expin, egain, routes, rweight, gateup, down,
    onehot, pos32, wsel32, combine, wide_t, send_b, xs, hs, y_b, ret,
    down_t, mout_t, grouped, prod_s, halo, outer_s,
    load_sem, disp_s, disp_r, ret_s, ret_r, ring_s, ring_r, part_s, part_r, halo_sem,
):
    ep = lax.axis_index("ep")
    tp = lax.axis_index("tp")
    z, x = ep // NX, lax.rem(ep, NX)
    core = lax.rem(tp, 2)
    mate = tp + 1 - 2 * core
    y_of = tp // 2

    def ep_at(dz, dx):
        return lax.rem(z + dz + NZ, NZ) * NX + lax.rem(x + dx + NX, NX)

    def ring_tp(d):
        return lax.rem(tp + 2 * d + N_TP, N_TP)

    loads = {}
    for i, (name, src, dst) in enumerate(
        [
            ("routes", routes_h, routes),
            ("expin", expin_h, expin),
            ("egain", egain_h, egain),
            ("mixin", mixin_h, mixin),
            ("mgain", mgain_h, mgain),
            ("outer", outer_h, mproj.at[pl.ds(0, 64)]),
            ("inner", inner_h, mproj.at[pl.ds(64, 64)]),
            ("value", value_h, mproj.at[pl.ds(128, 64)]),
            ("conv", conv_h, conv),
            ("ggain", ggain_h, ggain),
            ("rweight", rweight_h, rweight),
            ("gate", gate_h, gateup.at[pl.ds(0, 224)]),
            ("up", up_h, gateup.at[pl.ds(224, 224)]),
            ("down", down_h, down),
            ("mout", mout_h, mout),
        ]
    ):
        loads[name] = pltpu.make_async_copy(src, dst, load_sem.at[i])
        loads[name].start()

    barrier = pltpu.get_barrier_semaphore()
    for dz, dx in OFFSETS[1:]:
        pl.semaphore_signal(barrier, inc=1, device_id=(ep_at(dz, dx), tp), device_id_type=MESH)
    for other in (ring_tp(1), ring_tp(-1), mate):
        pl.semaphore_signal(barrier, inc=1, device_id=(ep, other), device_id_type=MESH)

    loads["routes"].wait()
    first, second = routes[0:1, :], routes[1:2, :]
    expert = lax.broadcasted_iota(jnp.int32, (N_EP, 256), 0)
    is_first = first == expert
    named = is_first | (second == expert)
    before = lax.broadcasted_iota(jnp.int32, (256, 256), 0) < lax.broadcasted_iota(
        jnp.int32, (256, 256), 1
    )
    rank = nn(jnp.where(named, 1.0, 0.0).astype(BF16), jnp.where(before, 1.0, 0.0).astype(BF16))
    pos32[...] = jnp.where(named, rank, -1.0)
    slot = lax.broadcasted_iota(jnp.int32, (CAP, 256), 0).astype(F32)
    for e in range(N_EP):
        onehot[e * CAP : (e + 1) * CAP, :] = jnp.where(slot == pos32[e : e + 1, :], 1.0, 0.0).astype(
            BF16
        )

    loads["expin"].wait()
    loads["egain"].wait()
    own_features = pl.ds(pl.multiple_of(tp * 128, 128), 128)
    rows = expin[...].astype(F32)
    scale = lax.rsqrt(jnp.mean(rows * rows, axis=-1, keepdims=True) + EPS)
    normed_b = (expin[:, own_features].astype(F32) * scale * egain[:, own_features]).astype(BF16)
    send_b[...] = nn(onehot[...], normed_b).astype(BF16)

    pl.semaphore_wait(barrier, N_EP - 1 + 3)

    def dispatch(b, i):
        dz, dx = GROUPS[b][i]
        target = ep_at(-dz, -dx)
        return pltpu.make_async_remote_copy(
            src_ref=send_b.at[pl.ds(pl.multiple_of(target * CAP, CAP), CAP)],
            dst_ref=xs.at[b, pl.ds(i * CAP, CAP), own_features],
            send_sem=disp_s.at[b, i],
            recv_sem=disp_r.at[b, i],
            device_id=(target, tp),
            device_id_type=MESH,
        )

    for b in range(BATCHES):
        for i, o in enumerate(GROUPS[b]):
            if o != (0, 0):
                dispatch(b, i).start()
            else:
                xs[b, i * CAP : (i + 1) * CAP, own_features] = send_b[
                    pl.ds(pl.multiple_of(ep * CAP, CAP), CAP), :
                ]

    for name in ("mixin", "mgain", "outer", "inner", "value"):
        loads[name].wait()
    rows_a = mixin[...].astype(F32)
    scale_a = lax.rsqrt(jnp.mean(rows_a * rows_a, axis=-1, keepdims=True) + EPS)
    normed_a = (rows_a * scale_a * mgain[...]).astype(BF16)
    projected = nt(mproj[...], normed_a).astype(BF16).astype(F32)
    outer_s[...] = projected[0:64]
    prod_s[...] = projected[64:128] * projected[128:192]
    next_ep = lax.rem(ep + 1, N_EP)
    halo_copy = pltpu.make_async_remote_copy(
        src_ref=prod_s,
        dst_ref=halo,
        send_sem=halo_sem.at[0],
        recv_sem=halo_sem.at[1],
        device_id=(next_ep, tp),
        device_id_type=MESH,
    )
    halo_copy.start()

    def mixer_group():
        halo_copy.wait()
        for name in ("conv", "ggain"):
            loads[name].wait()
        product = prod_s[...]
        behind = jnp.where(ep > 0, halo[...], 0.0)
        lane = lax.broadcasted_iota(jnp.int32, (64, 128), 1)
        one = jnp.where(lane < 1, pltpu.roll(behind, 1, 1), pltpu.roll(product, 1, 1))
        two = jnp.where(lane < 2, pltpu.roll(behind, 2, 1), pltpu.roll(product, 2, 1))
        mask = eye(64)
        taps = [column(conv[i : i + 1, :].astype(F32), mask) for i in range(3)]
        conv_sum = taps[0] * two + taps[1] * one + taps[2] * product
        gated = outer_s[...] * conv_sum
        norm = lax.rsqrt(jnp.mean(gated * gated, axis=0, keepdims=True) + EPS)
        own = pl.ds(pl.multiple_of(tp * 64, 64), 64)
        grouped[own, :] = (gated * norm * column(ggain[...], mask)).astype(BF16)

    def prepare_combine():
        loads["rweight"].wait()
        weight = jnp.where(is_first, rweight[0:1, :], rweight[1:2, :])
        high = weight.astype(BF16).astype(F32)
        identity = jnp.where(eye(256), 1.0, 0.0).astype(BF16)
        for part, value in enumerate((high, weight - high)):
            wsel32[...] = value
            for e in range(N_EP):
                wide_t[e * CAP : (e + 1) * CAP, :] = jnp.where(
                    slot == pos32[e : e + 1, :], wsel32[e : e + 1, :], 0.0
                ).astype(BF16)
            combine[part] = nt(identity, wide_t[...]).astype(BF16)

    def prepare_down():
        loads["down"].wait()
        identity = jnp.where(eye(128), 1.0, 0.0).astype(BF16)
        down_t[...] = nt(identity, down[...]).astype(BF16)
        loads["mout"].wait()
        mout_t[...] = nt(identity, mout[...]).astype(BF16)

    def piece_of(kind, b):
        if kind == "x":
            return lambda j: xs.at[b, :, pl.ds(pl.multiple_of(j * 128, 128), 128)]
        if kind == "h":
            return lambda j: hs.at[b, pl.ds(pl.multiple_of(j * 224, 224), 224)]
        return lambda j: grouped.at[pl.ds(pl.multiple_of(j * 64, 64), 64)]

    started = []

    def send(src, dst, send_sem, recv_sem, to):
        copy = pltpu.make_async_remote_copy(
            src_ref=src, dst_ref=dst, send_sem=send_sem, recv_sem=recv_sem,
            device_id=(ep, to), device_id_type=MESH,
        )
        copy.start()
        started.append(copy)

    class Gather:
        def __init__(self, number, kind, b, far):
            self.n, self.piece = number, piece_of(kind, b)
            self.reach = {1: 4 if far > 0 else 3, -1: 4 if far < 0 else 3}

        def index(self, way, k):
            return k - 1 if way == 1 else self.reach[1] + k - 1

        def on_ring(self, ref, way, k):
            i = self.index(way, k)
            send(ref, ref, ring_s.at[self.n, i], ring_r.at[self.n, i], ring_tp(way))

        def to_mate(self, ref, i):
            send(ref, ref, part_s.at[self.n, i], part_r.at[self.n, i], mate)

        def wait(self, ref, sem):
            pltpu.make_async_remote_copy(
                src_ref=ref, dst_ref=ref, send_sem=part_s.at[self.n, 0], recv_sem=sem,
                device_id=(ep, mate), device_id_type=MESH,
            ).wait_recv()

        def first(self):
            ref = self.piece(tp)
            self.on_ring(ref, 1, 1)
            self.on_ring(ref, -1, 1)
            self.to_mate(ref, 7)

        def step(self, k):
            for way in (1, -1):
                if k > self.reach[way]:
                    continue
                ref = self.piece(ring_tp(-way * k))
                i = self.index(way, k)
                self.wait(ref, ring_r.at[self.n, i])
                if k < self.reach[way]:
                    self.on_ring(ref, way, k + 1)
                self.to_mate(ref, i)

        def finish(self):
            self.wait(self.piece(mate), part_r.at[self.n, 7])
            for way in (1, -1):
                for k in range(1, self.reach[way] + 1):
                    j = lax.rem(mate - 2 * way * k + N_TP, N_TP)
                    self.wait(self.piece(j), part_r.at[self.n, self.index(way, k)])

    def wait_dispatched(b):
        for i, o in enumerate(GROUPS[b]):
            if o != (0, 0):
                dispatch(b, i).wait_recv()

    def hidden(b):
        both = nt(gateup[...], xs[b])
        gate, up = both[0:224], both[224:448]
        own = pl.ds(pl.multiple_of(tp * 224, 224), 224)
        hs[b, own, :] = (gate / (1.0 + jnp.exp(-gate)) * up).astype(BF16)

    def give_back(b, i):
        dz, dx = GROUPS[b][i]
        target = ep_at(dz, dx)
        return pltpu.make_async_remote_copy(
            src_ref=y_b.at[b, pl.ds(i * CAP, CAP)],
            dst_ref=ret.at[pl.ds(pl.multiple_of(ep * CAP, CAP), CAP)],
            send_sem=ret_s.at[b, i],
            recv_sem=ret_r.at[b, i],
            device_id=(target, tp),
            device_id_type=MESH,
        )

    def expert_result(b):
        out_t = nn(down_t[...], hs[b]).astype(BF16)
        identity = jnp.where(eye(256), 1.0, 0.0).astype(BF16)
        y_b[b] = nt(identity, out_t).astype(BF16)
        for i, o in enumerate(GROUPS[b]):
            if o != (0, 0):
                give_back(b, i).start()
            else:
                ret[pl.ds(pl.multiple_of(ep * CAP, CAP), CAP), :] = y_b[b, i * CAP : (i + 1) * CAP, :]

    def mixed_result():
        mixed_t = nn(mout_t[...], grouped[...]).astype(BF16)
        identity = jnp.where(eye(128), 1.0, 0.0).astype(BF16)
        mixed_o[...] = nt(identity, mixed_t).astype(BF16)

    def wait_weights():
        loads["gate"].wait()
        loads["up"].wait()

    tasks = []

    def at(slot_time, *calls):
        tasks.append((slot_time, len(tasks), calls))

    def gather_at(start, spacing, gather, before_calls, after_calls, gap):
        at(start, *before_calls, gather.first)
        for k in range(1, 5):
            at(start + spacing * k, functools.partial(gather.step, k))
        at(start + spacing * 4 + gap, gather.finish, *after_calls)

    at(0.1, wait_weights)
    at(0.2, prepare_combine)
    at(1.1, prepare_down)
    for b in range(BATCHES):
        way = 1 if b % 2 == 0 else -1
        gather_at(
            4 * b, 3, Gather(b, "x", b, way),
            [functools.partial(wait_dispatched, b)], [functools.partial(hidden, b)], 1.5,
        )
        gather_at(
            4 * (BATCHES + b), 3, Gather(BATCHES + b, "h", b, way),
            [], [functools.partial(expert_result, b)], 1.5,
        )
    gather_at(5.2, 3, Gather(2 * BATCHES, "m", 0, 1), [mixer_group], [mixed_result], 1.5)
    for _, _, calls in sorted(tasks, key=lambda task: task[:2]):
        for call in calls:
            call()

    for b in range(BATCHES):
        for i, o in enumerate(GROUPS[b]):
            if o != (0, 0):
                dz, dx = o
                source = ep_at(-dz, -dx)
                pltpu.make_async_remote_copy(
                    src_ref=y_b.at[b, pl.ds(i * CAP, CAP)],
                    dst_ref=ret.at[pl.ds(pl.multiple_of(source * CAP, CAP), CAP)],
                    send_sem=ret_s.at[b, i],
                    recv_sem=ret_r.at[b, i],
                    device_id=(source, tp),
                    device_id_type=MESH,
                ).wait_recv()
    results = ret[...]
    tokens_o[...] = (nn(combine[0], results) + nn(combine[1], results)).astype(BF16)

    for copy in started:
        copy.wait_send()
    for b in range(BATCHES):
        for i, o in enumerate(GROUPS[b]):
            if o != (0, 0):
                dispatch(b, i).wait_send()
                give_back(b, i).wait_send()


def per_device(
    mixer_input, mixer_gain, outer_weight, inner_weight, value_weight, conv_kernel, group_gain,
    mixer_out_weight, expert_input, expert_gain, routes, route_weight, expert_gate, expert_up,
    expert_down,
):
    phases = 2 * BATCHES + 1
    vmem = pltpu.VMEM
    dma = pltpu.SemaphoreType.DMA
    return pl.pallas_call(
        kernel,
        name="mixer_and_experts",
        out_shape=(
            jax.ShapeDtypeStruct((128, 128), BF16),
            jax.ShapeDtypeStruct((256, 128), BF16),
        ),
        in_specs=[pl.BlockSpec(memory_space=pl.ANY)] * 15,
        out_specs=(pl.BlockSpec(memory_space=vmem), pl.BlockSpec(memory_space=vmem)),
        scratch_shapes=[
            vmem((128, 2048), BF16),
            vmem((1, 2048), F32),
            vmem((192, 2048), BF16),
            vmem((3, 64), BF16),
            vmem((1, 64), F32),
            vmem((1024, 128), BF16),
            vmem((256, 2048), BF16),
            vmem((1, 2048), F32),
            vmem((2, 256), jnp.int32),
            vmem((2, 256), F32),
            vmem((448, 2048), BF16),
            vmem((3584, 128), BF16),
            vmem((1024, 256), BF16),
            vmem((N_EP, 256), F32),
            vmem((N_EP, 256), F32),
            vmem((2, 256, 1024), BF16),
            vmem((1024, 256), BF16),
            vmem((1024, 128), BF16),
            vmem((BATCHES, 256, 2048), BF16),
            vmem((BATCHES, 3584, 256), BF16),
            vmem((BATCHES, 256, 128), BF16),
            vmem((1024, 128), BF16),
            vmem((128, 3584), BF16),
            vmem((128, 1024), BF16),
            vmem((1024, 128), BF16),
            vmem((64, 128), F32),
            vmem((64, 128), F32),
            vmem((64, 128), F32),
            dma((15,)),
            dma((BATCHES, PER)),
            dma((BATCHES, PER)),
            dma((BATCHES, PER)),
            dma((BATCHES, PER)),
            dma((phases, 7)),
            dma((phases, 7)),
            dma((phases, 8)),
            dma((phases, 8)),
            dma((2,)),
        ],
        compiler_params=pltpu.CompilerParams(
            collective_id=0, has_side_effects=True, vmem_limit_bytes=56 * 1024 * 1024
        ),
    )(
        mixer_input, mixer_gain.reshape(1, -1), outer_weight.T, inner_weight.T, value_weight.T,
        conv_kernel, group_gain.reshape(1, -1), mixer_out_weight, expert_input,
        expert_gain.reshape(1, -1), routes.T, route_weight.T, expert_gate[0].T, expert_up[0].T,
        expert_down[0],
    )


def solution(mesh):
    placed = (
        P("ep", None), P(), P(None, "tp"), P(None, "tp"), P(None, "tp"), P(None, "tp"), P("tp"),
        P(None, "tp"), P("ep", None), P(), P("ep", None), P("ep", None), P("ep", None, "tp"),
        P("ep", None, "tp"), P("ep", None, "tp"),
    )
    return jax.shard_map(
        per_device,
        mesh=mesh,
        in_specs=placed,
        out_specs=(P("ep", "tp"), P("ep", "tp")),
        check_vma=False,
    )
```

```python
import functools

import jax
import jax.numpy as jnp
from jax import lax
from jax.experimental import pallas as pl
from jax.experimental.pallas import tpu as pltpu
from jax.sharding import PartitionSpec as P

EPS = 1e-06
MESH = pl.DeviceIdType.MESH
F32 = jnp.float32
BF16 = jnp.bfloat16
NZ, NX = 8, 4
N_EP = NZ * NX
N_Y = 8
N_TP = 2 * N_Y
BATCHES = 4
EARLY = 2
ROWS, HIDDEN, MIXER = "x", "h", "m"
END = 9
ORDER = (
    (ROWS, 0, 0), (ROWS, 1, 0), (ROWS, 0, 1), (ROWS, 0, 2), (ROWS, 1, 1), (ROWS, 2, 0),
    (ROWS, 1, 2), (ROWS, 0, 3), (ROWS, 0, END), (ROWS, 1, 3), (MIXER, 0, 0), (ROWS, 2, 1),
    (ROWS, 1, END), (ROWS, 2, 2), (HIDDEN, 1, 0), (ROWS, 2, 3), (ROWS, 3, 0), (ROWS, 2, END),
    (MIXER, 0, 1), (HIDDEN, 1, 1), (ROWS, 3, 1), (ROWS, 3, 2), (HIDDEN, 1, 2), (MIXER, 0, 2),
    (ROWS, 3, 3), (ROWS, 3, END), (HIDDEN, 3, 0), (HIDDEN, 2, 0), (HIDDEN, 1, 3), (MIXER, 0, 3),
    (HIDDEN, 3, 1), (HIDDEN, 0, 0), (HIDDEN, 2, 1), (HIDDEN, 1, 4), (HIDDEN, 1, END), (HIDDEN, 3, 2),
    (MIXER, 0, 4), (HIDDEN, 0, 1), (MIXER, 0, END), (HIDDEN, 2, 2), (HIDDEN, 3, 3), (HIDDEN, 0, 2),
    (HIDDEN, 2, 3), (HIDDEN, 3, 4), (HIDDEN, 3, END), (HIDDEN, 0, 3), (HIDDEN, 2, 4), (HIDDEN, 2, END),
    (HIDDEN, 0, 4), (HIDDEN, 0, END),
)
CAP = 32
PER = N_EP // BATCHES


GROUPS = (
    ((0, 0), (0, 1), (0, 2), (0, 3), (1, 0), (1, 1), (7, 0), (7, 3)),
    ((1, 2), (1, 3), (7, 1), (7, 2), (2, 0), (2, 1), (6, 0), (6, 3)),
    ((2, 2), (2, 3), (6, 1), (6, 2), (3, 0), (3, 1), (5, 0), (5, 3)),
    ((3, 2), (3, 3), (5, 1), (5, 2), (4, 0), (4, 1), (4, 2), (4, 3)),
)
COPIES = (2, 2, 2, 2)


def nt(a, b):
    return lax.dot_general(a, b, (((1,), (1,)), ((), ())), preferred_element_type=F32)


def nn(a, b):
    return lax.dot_general(a, b, (((1,), (0,)), ((), ())), preferred_element_type=F32)


def eye(n):
    return (
        lax.broadcasted_iota(jnp.int32, (n, n), 0) == lax.broadcasted_iota(jnp.int32, (n, n), 1)
    )


def column(row, mask):
    return jnp.sum(jnp.where(mask, row, 0.0), axis=1, keepdims=True)


def kernel(
    mixin_h, mgain_h, outer_h, inner_h, value_h, conv_h, ggain_h, mout_h,
    expin_h, egain_h, routes_h, rweight_h, gate_h, up_h, down_h,
    mixed_o, tokens_o,
    mixin, mgain, mproj, conv, ggain, mout,
    expin, egain, routes, rweight, gateup, down,
    onehot, pos32, wsel32, combine, wide_t, send_b, xs, hs, y_b, ret,
    down_t, mout_t, grouped, prod_s, halo, outer_s,
    load_sem, disp_s, disp_r, ret_s, ret_r, sent, ring_r, part_r, halo_sem,
):
    ep = lax.axis_index("ep")
    tp = lax.axis_index("tp")
    z, x = ep // NX, lax.rem(ep, NX)
    core = lax.rem(tp, 2)
    mate = tp + 1 - 2 * core
    y_of = tp // 2

    def ep_at(dz, dx):
        return lax.rem(z + dz + NZ, NZ) * NX + lax.rem(x + dx + NX, NX)

    def ring_tp(d):
        return lax.rem(tp + 2 * d + N_TP, N_TP)

    across = ring_tp(N_Y // 2)

    def features(j):
        return pl.ds(pl.multiple_of(j * 128, 128), 128)

    sources = dict(
        routes=(routes_h, routes),
        expin=(expin_h, expin),
        egain=(egain_h, egain),
        mixin=(mixin_h, mixin),
        mgain=(mgain_h, mgain),
        outer=(outer_h, mproj.at[pl.ds(0, 64)]),
        inner=(inner_h, mproj.at[pl.ds(64, 64)]),
        value=(value_h, mproj.at[pl.ds(128, 64)]),
        conv=(conv_h, conv),
        ggain=(ggain_h, ggain),
        rweight=(rweight_h, rweight),
        gate=(gate_h, gateup.at[pl.ds(0, 224)]),
        up=(up_h, gateup.at[pl.ds(224, 224)]),
        down=(down_h, down),
        mout=(mout_h, mout),
    )
    loads = {
        name: pltpu.make_async_copy(src, dst, load_sem.at[i])
        for i, (name, (src, dst)) in enumerate(sources.items())
    }
    urgent = ("routes", "expin", "egain")
    for name in urgent:
        loads[name].start()

    barrier = pltpu.get_barrier_semaphore()
    for dz, dx in (o for group in GROUPS for o in group if o != (0, 0)):
        pl.semaphore_signal(barrier, inc=1, device_id=(ep_at(dz, dx), tp), device_id_type=MESH)
    for other in (ring_tp(1), ring_tp(-1), mate):
        pl.semaphore_signal(barrier, inc=1, device_id=(ep, other), device_id_type=MESH)

    loads["routes"].wait()
    first, second = routes[0:1, :], routes[1:2, :]
    expert = lax.broadcasted_iota(jnp.int32, (N_EP, 256), 0)
    is_first = first == expert
    named = is_first | (second == expert)
    before = lax.broadcasted_iota(jnp.int32, (256, 256), 0) < lax.broadcasted_iota(
        jnp.int32, (256, 256), 1
    )
    rank = nn(jnp.where(named, 1.0, 0.0).astype(BF16), jnp.where(before, 1.0, 0.0).astype(BF16))
    pos32[...] = jnp.where(named, rank, -1.0)
    slot = lax.broadcasted_iota(jnp.int32, (CAP, 256), 0).astype(F32)
    for e in range(N_EP):
        onehot[e * CAP : (e + 1) * CAP, :] = jnp.where(slot == pos32[e : e + 1, :], 1.0, 0.0).astype(
            BF16
        )

    loads["expin"].wait()
    loads["egain"].wait()
    for name in loads:
        if name not in urgent:
            loads[name].start()
    rows = expin[...].astype(F32)
    scale = lax.rsqrt(jnp.mean(rows * rows, axis=-1, keepdims=True) + EPS)
    normed_b = jnp.concatenate(
        [
            (expin[:, part].astype(F32) * scale * egain[:, part]).astype(BF16)
            for part in (features(tp), features(across))
        ],
        axis=1,
    )
    both_parts = nn(onehot[...], normed_b).astype(BF16)
    send_b[0], send_b[1] = both_parts[:, :128], both_parts[:, 128:]

    pl.semaphore_wait(barrier, N_EP - 1 + 3)

    def dispatch(b, i, part):
        dz, dx = GROUPS[b][i]
        target = ep_at(-dz, -dx)
        return pltpu.make_async_remote_copy(
            src_ref=send_b.at[part, pl.ds(pl.multiple_of(target * CAP, CAP), CAP)],
            dst_ref=xs.at[b, pl.ds(i * CAP, CAP), features((tp, across)[part])],
            send_sem=disp_s.at[0],
            recv_sem=disp_r.at[b],
            device_id=(target, tp),
            device_id_type=MESH,
        )

    def dispatch_batch(b):
        for i, o in enumerate(GROUPS[b]):
            for part, chunk in enumerate((tp, across)[: COPIES[b]]):
                if o != (0, 0):
                    dispatch(b, i, part).start()
                else:
                    xs[b, i * CAP : (i + 1) * CAP, features(chunk)] = send_b[
                        part, pl.ds(pl.multiple_of(ep * CAP, CAP), CAP), :
                    ]

    for b in range(EARLY):
        dispatch_batch(b)

    for name in ("mixin", "mgain", "outer", "inner", "value"):
        loads[name].wait()
    rows_a = mixin[...].astype(F32)
    scale_a = lax.rsqrt(jnp.mean(rows_a * rows_a, axis=-1, keepdims=True) + EPS)
    normed_a = (rows_a * scale_a * mgain[...]).astype(BF16)
    projected = nt(mproj[...], normed_a).astype(BF16).astype(F32)
    outer_s[...] = projected[0:64]
    prod_s[...] = projected[64:128] * projected[128:192]
    next_ep = lax.rem(ep + 1, N_EP)
    halo_copy = pltpu.make_async_remote_copy(
        src_ref=prod_s,
        dst_ref=halo,
        send_sem=halo_sem.at[0],
        recv_sem=halo_sem.at[1],
        device_id=(next_ep, tp),
        device_id_type=MESH,
    )
    halo_copy.start()
    for b in range(EARLY, BATCHES):
        dispatch_batch(b)

    def mixer_group():
        halo_copy.wait()
        for name in ("conv", "ggain"):
            loads[name].wait()
        product = prod_s[...]
        behind = jnp.where(ep > 0, halo[...], 0.0)
        lane = lax.broadcasted_iota(jnp.int32, (64, 128), 1)
        one = jnp.where(lane < 1, pltpu.roll(behind, 1, 1), pltpu.roll(product, 1, 1))
        two = jnp.where(lane < 2, pltpu.roll(behind, 2, 1), pltpu.roll(product, 2, 1))
        mask = eye(64)
        taps = [column(conv[i : i + 1, :].astype(F32), mask) for i in range(3)]
        conv_sum = taps[0] * two + taps[1] * one + taps[2] * product
        gated = outer_s[...] * conv_sum
        norm = lax.rsqrt(jnp.mean(gated * gated, axis=0, keepdims=True) + EPS)
        own = pl.ds(pl.multiple_of(tp * 64, 64), 64)
        grouped[own, :] = (gated * norm * column(ggain[...], mask)).astype(BF16)

    def prepare_combine():
        loads["rweight"].wait()
        weight = jnp.where(is_first, rweight[0:1, :], rweight[1:2, :])
        high = weight.astype(BF16).astype(F32)
        identity = jnp.where(eye(256), 1.0, 0.0).astype(BF16)
        for part, value in enumerate((high, weight - high)):
            wsel32[...] = value
            for e in range(N_EP):
                wide_t[e * CAP : (e + 1) * CAP, :] = jnp.where(
                    slot == pos32[e : e + 1, :], wsel32[e : e + 1, :], 0.0
                ).astype(BF16)
            combine[part] = nt(identity, wide_t[...]).astype(BF16)

    def prepare_down():
        loads["down"].wait()
        identity = jnp.where(eye(128), 1.0, 0.0).astype(BF16)
        down_t[...] = nt(identity, down[...]).astype(BF16)
        loads["mout"].wait()
        mout_t[...] = nt(identity, mout[...]).astype(BF16)

    def piece_of(kind, b):
        if kind == ROWS:
            return lambda j, h=0, n=1: xs.at[b, pl.ds(h * 128, 256 // n), features(j)]
        if kind == HIDDEN:
            return lambda j, h=0, n=1: hs.at[b, pl.ds(pl.multiple_of(j * 224 + h * 112, 16), 224 // n)]
        return lambda j, h=0, n=1: grouped.at[pl.ds(pl.multiple_of(j * 64 + h * 32, 32), 64 // n)]

    def part_of(kind, b):
        if kind == ROWS:
            return lambda n: xs.at[b, :, pl.ds(0, n * 128)]
        if kind == HIDDEN:
            return lambda n: hs.at[b, pl.ds(0, n * 224)]
        return lambda n: grouped.at[pl.ds(0, n * 64)]

    def arrived(ref, sem):
        pltpu.make_async_remote_copy(
            src_ref=ref, dst_ref=ref, send_sem=disp_s.at[0], recv_sem=sem,
            device_id=(ep, mate), device_id_type=MESH,
        ).wait_recv()

    def left(ref, sem):
        pltpu.make_async_remote_copy(
            src_ref=ref, dst_ref=ref, send_sem=sem, recv_sem=disp_r.at[0],
            device_id=(ep, mate), device_id_type=MESH,
        ).wait_send()

    def remote_rows(b):
        return CAP * sum(o != (0, 0) for o in GROUPS[b])

    def send(src, dst, send_sem, recv_sem, to):
        copy = pltpu.make_async_remote_copy(
            src_ref=src, dst_ref=dst, send_sem=send_sem, recv_sem=recv_sem,
            device_id=(ep, to), device_id_type=MESH,
        )
        copy.start()

    class Gather:
        def __init__(self, number, kind, b):
            self.n, self.piece, self.part = number, piece_of(kind, b), part_of(kind, b)

        def received(self, way, k):
            return ring_r.at[self.n, (k if way == 1 else 4 + k) - 1]

        def on_ring(self, ref, way, k):
            send(ref, ref, sent.at[self.n], self.received(way, k), ring_tp(way))

        def to_mate(self, ref):
            send(ref, ref, sent.at[self.n], part_r.at[self.n], mate)

        def first(self):
            ref = self.piece(tp)
            self.on_ring(ref, 1, 1)
            self.on_ring(ref, -1, 1)
            self.to_mate(ref)

        def step(self, k):
            for way, h in ((1, 0), (-1, 1)):
                j = ring_tp(-way * k)
                ref = self.piece(j) if k < 4 else self.piece(j, h, 2)
                arrived(ref, self.received(way, k))
                if k < 4:
                    self.on_ring(ref if k < 3 else self.piece(j, h, 2), way, k + 1)
                self.to_mate(ref)

        def finish(self):
            arrived(self.part(N_Y), part_r.at[self.n])

        def all_sent(self):
            left(self.part(N_TP - 1), sent.at[self.n])

    class PairGather(Gather):
        def first(self):
            for k, j in enumerate((tp, across)):
                ref = self.piece(j)
                self.on_ring(ref, 1, 1 + k)
                self.on_ring(ref, -1, 1 + k)
                self.to_mate(ref)

        def step(self, k):
            for way in (1, -1):
                ref = self.piece(ring_tp((-way, 3 * way, -2 * way)[k - 1]))
                arrived(ref, self.received(way, k))
                if k == 1:
                    self.on_ring(ref, way, 3)
                self.to_mate(ref)

        def all_sent(self):
            left(self.part(N_TP - 2), sent.at[self.n])

    def wait_dispatched(b):
        arrived(xs.at[b, pl.ds(0, remote_rows(b)), pl.ds(0, 128 * COPIES[b])], disp_r.at[b])

    def hidden(b):
        both = nt(gateup[...], xs[b])
        gate, up = both[0:224], both[224:448]
        own = pl.ds(pl.multiple_of(tp * 224, 224), 224)
        hs[b, own, :] = (gate / (1.0 + jnp.exp(-gate)) * up).astype(BF16)

    def give_back(b, i):
        dz, dx = GROUPS[b][i]
        target = ep_at(dz, dx)
        return pltpu.make_async_remote_copy(
            src_ref=y_b.at[b, pl.ds(i * CAP, CAP)],
            dst_ref=ret.at[pl.ds(pl.multiple_of(ep * CAP, CAP), CAP)],
            send_sem=ret_s.at[0],
            recv_sem=ret_r.at[0],
            device_id=(target, tp),
            device_id_type=MESH,
        )

    def expert_result(b):
        out_t = nn(down_t[...], hs[b]).astype(BF16)
        identity = jnp.where(eye(256), 1.0, 0.0).astype(BF16)
        y_b[b] = nt(identity, out_t).astype(BF16)
        for i, o in enumerate(GROUPS[b]):
            if o != (0, 0):
                give_back(b, i).start()
            else:
                ret[pl.ds(pl.multiple_of(ep * CAP, CAP), CAP), :] = y_b[b, i * CAP : (i + 1) * CAP, :]

    def mixed_result():
        mixed_t = nn(mout_t[...], grouped[...]).astype(BF16)
        identity = jnp.where(eye(128), 1.0, 0.0).astype(BF16)
        mixed_o[...] = nt(identity, mixed_t).astype(BF16)

    def wait_weights():
        loads["gate"].wait()
        loads["up"].wait()

    gathers = {(MIXER, 0): Gather(2 * BATCHES, MIXER, 0)}
    for b in range(BATCHES):
        gathers[ROWS, b] = (PairGather if COPIES[b] == 2 else Gather)(b, ROWS, b)
        gathers[HIDDEN, b] = Gather(BATCHES + b, HIDDEN, b)

    for kind, b, step in ORDER:
        gather = gathers[kind, b]
        if step == 0:
            if kind == ROWS:
                wait_dispatched(b)
            elif kind == MIXER:
                mixer_group()
            gather.first()
            if kind == ROWS and b == 0:
                wait_weights()
                prepare_combine()
            elif kind == ROWS and b == 1:
                prepare_down()
        elif step < END:
            gather.step(step)
        else:
            gather.finish()
            if kind == ROWS:
                hidden(b)
            elif kind == HIDDEN:
                expert_result(b)
            else:
                mixed_result()

    others = (N_EP - 1) * CAP
    arrived(ret.at[pl.ds(0, others)], ret_r.at[0])
    results = ret[...]
    tokens_o[...] = (nn(combine[0], results) + nn(combine[1], results)).astype(BF16)

    for gather in gathers.values():
        gather.all_sent()
    for b in range(BATCHES):
        for _ in range(COPIES[b]):
            left(send_b.at[0, pl.ds(0, remote_rows(b))], disp_s.at[0])
    left(ret.at[pl.ds(0, others)], ret_s.at[0])


def per_device(
    mixer_input, mixer_gain, outer_weight, inner_weight, value_weight, conv_kernel, group_gain,
    mixer_out_weight, expert_input, expert_gain, routes, route_weight, expert_gate, expert_up,
    expert_down,
):
    phases = 2 * BATCHES + 1
    vmem = pltpu.VMEM
    dma = pltpu.SemaphoreType.DMA
    return pl.pallas_call(
        kernel,
        name="mixer_and_experts",
        out_shape=(
            jax.ShapeDtypeStruct((128, 128), BF16),
            jax.ShapeDtypeStruct((256, 128), BF16),
        ),
        in_specs=[pl.BlockSpec(memory_space=pl.ANY)] * 15,
        out_specs=(pl.BlockSpec(memory_space=vmem), pl.BlockSpec(memory_space=vmem)),
        scratch_shapes=[
            vmem((128, 2048), BF16),
            vmem((1, 2048), F32),
            vmem((192, 2048), BF16),
            vmem((3, 64), BF16),
            vmem((1, 64), F32),
            vmem((1024, 128), BF16),
            vmem((256, 2048), BF16),
            vmem((1, 2048), F32),
            vmem((2, 256), jnp.int32),
            vmem((2, 256), F32),
            vmem((448, 2048), BF16),
            vmem((3584, 128), BF16),
            vmem((1024, 256), BF16),
            vmem((N_EP, 256), F32),
            vmem((N_EP, 256), F32),
            vmem((2, 256, 1024), BF16),
            vmem((1024, 256), BF16),
            vmem((2, 1024, 128), BF16),
            vmem((BATCHES, 256, 2048), BF16),
            vmem((BATCHES, 3584, 256), BF16),
            vmem((BATCHES, 256, 128), BF16),
            vmem((1024, 128), BF16),
            vmem((128, 3584), BF16),
            vmem((128, 1024), BF16),
            vmem((1024, 128), BF16),
            vmem((64, 128), F32),
            vmem((64, 128), F32),
            vmem((64, 128), F32),
            dma((15,)),
            dma((1,)),
            dma((BATCHES,)),
            dma((1,)),
            dma((1,)),
            dma((phases,)),
            dma((phases, 8)),
            dma((phases,)),
            dma((2,)),
        ],
        compiler_params=pltpu.CompilerParams(
            collective_id=0, has_side_effects=True, vmem_limit_bytes=56 * 1024 * 1024
        ),
    )(
        mixer_input, mixer_gain.reshape(1, -1), outer_weight.T, inner_weight.T, value_weight.T,
        conv_kernel, group_gain.reshape(1, -1), mixer_out_weight, expert_input,
        expert_gain.reshape(1, -1), routes.T, route_weight.T, expert_gate[0].T, expert_up[0].T,
        expert_down[0],
    )


def solution(mesh):
    placed = (
        P("ep", None), P(), P(None, "tp"), P(None, "tp"), P(None, "tp"), P(None, "tp"), P("tp"),
        P(None, "tp"), P("ep", None), P(), P("ep", None), P("ep", None), P("ep", None, "tp"),
        P("ep", None, "tp"), P("ep", None, "tp"),
    )
    return jax.shard_map(
        per_device,
        mesh=mesh,
        in_specs=placed,
        out_specs=(P("ep", "tp"), P("ep", "tp")),
        check_vma=False,
    )
```

```python
import functools

import jax
import jax.numpy as jnp
from jax import lax
from jax.experimental import pallas as pl
from jax.experimental.pallas import tpu as pltpu
from jax.sharding import PartitionSpec as P

EPS = 1e-06
MESH = pl.DeviceIdType.MESH
F32 = jnp.float32
BF16 = jnp.bfloat16
NZ, NX = 8, 4
N_EP = NZ * NX
N_Y = 8
N_TP = 2 * N_Y
BATCHES = 4
EARLY = 2
ROWS, HIDDEN, MIXER = "x", "h", "m"
END = 9
ORDER = (
    (ROWS, 0, 0), (ROWS, 1, 0), (ROWS, 0, 1), (ROWS, 1, 1), (ROWS, 0, 2), (ROWS, 2, 0),
    (ROWS, 1, 2), (ROWS, 3, 0), (ROWS, 1, 3), (ROWS, 2, 1), (ROWS, 1, END), (ROWS, 0, 3),
    (ROWS, 3, 1), (ROWS, 2, 2), (HIDDEN, 1, 0), (ROWS, 0, END), (HIDDEN, 0, 0), (ROWS, 3, 2),
    (ROWS, 2, 3), (ROWS, 2, END), (ROWS, 3, 3), (HIDDEN, 2, 0), (ROWS, 3, END), (HIDDEN, 3, 0),
    (HIDDEN, 1, 1), (HIDDEN, 2, 1), (HIDDEN, 3, 1), (MIXER, 0, 0), (HIDDEN, 1, 2), (HIDDEN, 3, 2),
    (HIDDEN, 0, 1), (HIDDEN, 2, 2), (HIDDEN, 3, 3), (HIDDEN, 0, 2), (MIXER, 0, 1), (HIDDEN, 2, 3),
    (HIDDEN, 1, 3), (HIDDEN, 3, 4), (HIDDEN, 0, 3), (HIDDEN, 3, END), (HIDDEN, 2, 4), (MIXER, 0, 2),
    (HIDDEN, 1, 4), (HIDDEN, 2, END), (HIDDEN, 0, 4), (HIDDEN, 1, END), (MIXER, 0, 3), (HIDDEN, 0, END),
    (MIXER, 0, 4), (MIXER, 0, END),
)
CAP = 32
PER = N_EP // BATCHES


GROUPS = (
    ((1, 0), (7, 0), (0, 1), (0, 3), (1, 1), (7, 3), (0, 2), (0, 0)),
    ((2, 0), (6, 0), (1, 3), (7, 1), (2, 1), (6, 3), (1, 2), (7, 2)),
    ((2, 2), (6, 2), (3, 0), (5, 0), (2, 3), (6, 1), (3, 1), (5, 3)),
    ((4, 0), (5, 1), (3, 3), (4, 1), (5, 2), (3, 2), (4, 3), (4, 2)),
)
COPIES = (2, 2, 2, 2)


def nt(a, b):
    return lax.dot_general(a, b, (((1,), (1,)), ((), ())), preferred_element_type=F32)


def nn(a, b):
    return lax.dot_general(a, b, (((1,), (0,)), ((), ())), preferred_element_type=F32)


def eye(n):
    return (
        lax.broadcasted_iota(jnp.int32, (n, n), 0) == lax.broadcasted_iota(jnp.int32, (n, n), 1)
    )


def column(row, mask):
    return jnp.sum(jnp.where(mask, row, 0.0), axis=1, keepdims=True)


def kernel(
    mixin_h, mgain_h, outer_h, inner_h, value_h, conv_h, ggain_h, mout_h,
    expin_h, egain_h, routes_h, rweight_h, gate_h, up_h, down_h,
    mixed_o, tokens_o,
    mixin, mgain, mproj, conv, ggain, mout,
    expin, egain, routes, rweight, gateup, down,
    onehot, pos32, wsel32, combine, wide_t, send_b, xs, hs, y_b, ret,
    down_t, mout_t, grouped, prod_s, halo, outer_s,
    load_sem, disp_s, disp_r, ret_s, ret_r, sent, ring_r, part_r, halo_sem,
):
    ep = lax.axis_index("ep")
    tp = lax.axis_index("tp")
    z, x = ep // NX, lax.rem(ep, NX)
    core = lax.rem(tp, 2)
    mate = tp + 1 - 2 * core
    y_of = tp // 2

    def ep_at(dz, dx):
        return lax.rem(z + dz + NZ, NZ) * NX + lax.rem(x + dx + NX, NX)

    def ring_tp(d):
        return lax.rem(tp + 2 * d + N_TP, N_TP)

    across = ring_tp(N_Y // 2)
    low = lax.rem(tp, N_Y)

    def features(j):
        return pl.ds(pl.multiple_of(j * 128, 128), 128)

    def place(j):
        return features(2 * lax.rem(j, N_Y) + j // N_Y)

    sources = dict(
        routes=(routes_h, routes),
        expin=(expin_h, expin),
        egain=(egain_h, egain),
        mixin=(mixin_h, mixin),
        mgain=(mgain_h, mgain),
        outer=(outer_h, mproj.at[pl.ds(0, 64)]),
        inner=(inner_h, mproj.at[pl.ds(64, 64)]),
        value=(value_h, mproj.at[pl.ds(128, 64)]),
        conv=(conv_h, conv),
        ggain=(ggain_h, ggain),
        rweight=(rweight_h, rweight),
        down=(down_h, down),
        mout=(mout_h, mout),
    )
    loads = {
        name: pltpu.make_async_copy(src, dst, load_sem.at[i])
        for i, (name, (src, dst)) in enumerate(sources.items())
    }
    urgent = ("routes", "expin", "egain")
    for name in urgent:
        loads[name].start()

    barrier = pltpu.get_barrier_semaphore()
    for dz, dx in (o for group in GROUPS for o in group if o != (0, 0)):
        pl.semaphore_signal(barrier, inc=1, device_id=(ep_at(dz, dx), tp), device_id_type=MESH)
    for other in (ring_tp(1), ring_tp(-1), mate):
        pl.semaphore_signal(barrier, inc=1, device_id=(ep, other), device_id_type=MESH)

    loads["routes"].wait()
    first, second = routes[0:1, :], routes[1:2, :]
    expert = lax.broadcasted_iota(jnp.int32, (N_EP, 256), 0)
    is_first = first == expert
    named = is_first | (second == expert)
    before = lax.broadcasted_iota(jnp.int32, (256, 256), 0) < lax.broadcasted_iota(
        jnp.int32, (256, 256), 1
    )
    rank = nn(jnp.where(named, 1.0, 0.0).astype(BF16), jnp.where(before, 1.0, 0.0).astype(BF16))
    pos32[...] = jnp.where(named, rank, -1.0)
    slot = lax.broadcasted_iota(jnp.int32, (CAP, 256), 0).astype(F32)
    for e in range(N_EP):
        onehot[e * CAP : (e + 1) * CAP, :] = jnp.where(slot == pos32[e : e + 1, :], 1.0, 0.0).astype(
            BF16
        )

    loads["expin"].wait()
    loads["egain"].wait()
    for name in loads:
        if name not in urgent:
            loads[name].start()
    for part, weight in enumerate((gate_h, up_h)):
        for j in range(N_TP):
            pltpu.make_async_copy(
                weight.at[:, pl.ds(j * 128, 128)],
                gateup.at[pl.ds(part * 224, 224), pl.ds((2 * (j % N_Y) + j // N_Y) * 128, 128)],
                load_sem.at[len(loads)],
            ).start()
    rows = expin[...].astype(F32)
    scale = lax.rsqrt(jnp.mean(rows * rows, axis=-1, keepdims=True) + EPS)
    normed_b = jnp.concatenate(
        [
            (expin[:, part].astype(F32) * scale * egain[:, part]).astype(BF16)
            for part in (features(low), features(low + N_Y))
        ],
        axis=1,
    )
    send_b[...] = nn(onehot[...], normed_b).astype(BF16)

    pl.semaphore_wait(barrier, N_EP - 1 + 3)

    def dispatch_parts(b, i, target):
        rows = pl.ds(pl.multiple_of(target * CAP, CAP), CAP)
        if COPIES[b] == 2:
            to = pl.ds(pl.multiple_of(low * 256, 256), 256)
            return send_b.at[rows], xs.at[b, pl.ds(i * CAP, CAP), to]
        return send_b.at[rows, features(tp // N_Y)], xs.at[b, pl.ds(i * CAP, CAP), place(tp)]

    def dispatch_batch(b):
        for i, (dz, dx) in enumerate(GROUPS[b]):
            target = ep_at(-dz, -dx)
            src, dst = dispatch_parts(b, i, target)
            if (dz, dx) == (0, 0):
                dst[...] = src[...]
            else:
                pltpu.make_async_remote_copy(
                    src_ref=src, dst_ref=dst, send_sem=disp_s.at[0], recv_sem=disp_r.at[b],
                    device_id=(target, tp), device_id_type=MESH,
                ).start()

    for b in range(EARLY):
        dispatch_batch(b)

    for name in ("mixin", "mgain", "outer", "inner", "value"):
        loads[name].wait()
    rows_a = mixin[...].astype(F32)
    scale_a = lax.rsqrt(jnp.mean(rows_a * rows_a, axis=-1, keepdims=True) + EPS)
    normed_a = (rows_a * scale_a * mgain[...]).astype(BF16)
    projected = nt(mproj[...], normed_a).astype(BF16).astype(F32)
    outer_s[...] = projected[0:64]
    prod_s[...] = projected[64:128] * projected[128:192]
    next_ep = lax.rem(ep + 1, N_EP)
    halo_copy = pltpu.make_async_remote_copy(
        src_ref=prod_s,
        dst_ref=halo,
        send_sem=halo_sem.at[0],
        recv_sem=halo_sem.at[1],
        device_id=(next_ep, tp),
        device_id_type=MESH,
    )
    halo_copy.start()
    for b in range(EARLY, BATCHES):
        dispatch_batch(b)

    def mixer_group():
        halo_copy.wait()
        for name in ("conv", "ggain"):
            loads[name].wait()
        product = prod_s[...]
        behind = jnp.where(ep > 0, halo[...], 0.0)
        lane = lax.broadcasted_iota(jnp.int32, (64, 128), 1)
        one = jnp.where(lane < 1, pltpu.roll(behind, 1, 1), pltpu.roll(product, 1, 1))
        two = jnp.where(lane < 2, pltpu.roll(behind, 2, 1), pltpu.roll(product, 2, 1))
        mask = eye(64)
        taps = [column(conv[i : i + 1, :].astype(F32), mask) for i in range(3)]
        conv_sum = taps[0] * two + taps[1] * one + taps[2] * product
        gated = outer_s[...] * conv_sum
        norm = lax.rsqrt(jnp.mean(gated * gated, axis=0, keepdims=True) + EPS)
        own = pl.ds(pl.multiple_of(tp * 64, 64), 64)
        grouped[own, :] = (gated * norm * column(ggain[...], mask)).astype(BF16)

    def prepare_combine():
        loads["rweight"].wait()
        weight = jnp.where(is_first, rweight[0:1, :], rweight[1:2, :])
        high = weight.astype(BF16).astype(F32)
        identity = jnp.where(eye(256), 1.0, 0.0).astype(BF16)
        for part, value in enumerate((high, weight - high)):
            wsel32[...] = value
            for e in range(N_EP):
                wide_t[e * CAP : (e + 1) * CAP, :] = jnp.where(
                    slot == pos32[e : e + 1, :], wsel32[e : e + 1, :], 0.0
                ).astype(BF16)
            combine[part] = nt(identity, wide_t[...]).astype(BF16)

    def prepare_down():
        loads["down"].wait()
        identity = jnp.where(eye(128), 1.0, 0.0).astype(BF16)
        down_t[...] = nt(identity, down[...]).astype(BF16)
        loads["mout"].wait()
        mout_t[...] = nt(identity, mout[...]).astype(BF16)

    def piece_of(kind, b):
        if kind == ROWS:
            return lambda j, h=0, n=1: xs.at[b, pl.ds(h * 128, 256 // n), place(j)]
        if kind == HIDDEN:
            return lambda j, h=0, n=1: hs.at[b, pl.ds(pl.multiple_of(j * 224 + h * 112, 16), 224 // n)]
        return lambda j, h=0, n=1: grouped.at[pl.ds(pl.multiple_of(j * 64 + h * 32, 32), 64 // n)]

    def part_of(kind, b):
        if kind == ROWS:
            return lambda n: xs.at[b, :, pl.ds(0, n * 128)]
        if kind == HIDDEN:
            return lambda n: hs.at[b, pl.ds(0, n * 224)]
        return lambda n: grouped.at[pl.ds(0, n * 64)]

    def arrived(ref, sem):
        pltpu.make_async_remote_copy(
            src_ref=ref, dst_ref=ref, send_sem=disp_s.at[0], recv_sem=sem,
            device_id=(ep, mate), device_id_type=MESH,
        ).wait_recv()

    def left(ref, sem):
        pltpu.make_async_remote_copy(
            src_ref=ref, dst_ref=ref, send_sem=sem, recv_sem=disp_r.at[0],
            device_id=(ep, mate), device_id_type=MESH,
        ).wait_send()

    def remote_rows(b):
        return CAP * sum(o != (0, 0) for o in GROUPS[b])

    def send(src, dst, send_sem, recv_sem, to):
        copy = pltpu.make_async_remote_copy(
            src_ref=src, dst_ref=dst, send_sem=send_sem, recv_sem=recv_sem,
            device_id=(ep, to), device_id_type=MESH,
        )
        copy.start()

    class Gather:
        def __init__(self, number, kind, b):
            self.n, self.piece, self.part = number, piece_of(kind, b), part_of(kind, b)

        def received(self, way, k):
            return ring_r.at[self.n, (k if way == 1 else 4 + k) - 1]

        def on_ring(self, ref, way, k):
            send(ref, ref, sent.at[self.n], self.received(way, k), ring_tp(way))

        def to_mate(self, ref):
            send(ref, ref, sent.at[self.n], part_r.at[self.n], mate)

        def first(self):
            ref = self.piece(tp)
            self.to_mate(ref)
            self.on_ring(ref, 1, 1)
            self.on_ring(ref, -1, 1)

        def step(self, k):
            for way, h in ((1, 0), (-1, 1)):
                j = ring_tp(-way * k)
                ref = self.piece(j) if k < 4 else self.piece(j, h, 2)
                arrived(ref, self.received(way, k))
                self.to_mate(ref)
                if k < 4:
                    self.on_ring(ref if k < 3 else self.piece(j, h, 2), way, k + 1)

        def finish(self):
            arrived(self.part(N_Y), part_r.at[self.n])

        def all_sent(self):
            left(self.part(N_TP - 1), sent.at[self.n])

    class PairGather(Gather):
        def first(self):
            for k, j in enumerate((tp, across)):
                ref = self.piece(j)
                self.to_mate(ref)
                self.on_ring(ref, 1, 1 + k)
                self.on_ring(ref, -1, 1 + k)

        def step(self, k):
            for way in (1, -1):
                ref = self.piece(ring_tp((-way, 3 * way, -2 * way)[k - 1]))
                arrived(ref, self.received(way, k))
                self.to_mate(ref)
                if k == 1:
                    self.on_ring(ref, way, 3)

        def all_sent(self):
            left(self.part(N_TP - 2), sent.at[self.n])

    def wait_dispatched(b):
        arrived(xs.at[b, pl.ds(0, remote_rows(b)), pl.ds(0, 128 * COPIES[b])], disp_r.at[b])

    def hidden(b):
        both = nt(gateup[...], xs[b])
        gate, up = both[0:224], both[224:448]
        own = pl.ds(pl.multiple_of(tp * 224, 224), 224)
        hs[b, own, :] = (gate / (1.0 + jnp.exp(-gate)) * up).astype(BF16)

    def give_back(b, i):
        dz, dx = GROUPS[b][i]
        target = ep_at(dz, dx)
        return pltpu.make_async_remote_copy(
            src_ref=y_b.at[b, pl.ds(i * CAP, CAP)],
            dst_ref=ret.at[pl.ds(pl.multiple_of(ep * CAP, CAP), CAP)],
            send_sem=ret_s.at[0],
            recv_sem=ret_r.at[0],
            device_id=(target, tp),
            device_id_type=MESH,
        )

    def expert_result(b):
        out_t = nn(down_t[...], hs[b]).astype(BF16)
        identity = jnp.where(eye(256), 1.0, 0.0).astype(BF16)
        y_b[b] = nt(identity, out_t).astype(BF16)
        for i, o in enumerate(GROUPS[b]):
            if o != (0, 0):
                give_back(b, i).start()
            else:
                ret[pl.ds(pl.multiple_of(ep * CAP, CAP), CAP), :] = y_b[b, i * CAP : (i + 1) * CAP, :]

    def mixed_result():
        mixed_t = nn(mout_t[...], grouped[...]).astype(BF16)
        identity = jnp.where(eye(128), 1.0, 0.0).astype(BF16)
        mixed_o[...] = nt(identity, mixed_t).astype(BF16)

    def wait_weights():
        pltpu.make_async_copy(gateup, gateup, load_sem.at[len(loads)]).wait()

    gathers = {(MIXER, 0): Gather(2 * BATCHES, MIXER, 0)}
    for b in range(BATCHES):
        gathers[ROWS, b] = (PairGather if COPIES[b] == 2 else Gather)(b, ROWS, b)
        gathers[HIDDEN, b] = Gather(BATCHES + b, HIDDEN, b)

    for kind, b, step in ORDER:
        gather = gathers[kind, b]
        if step == 0:
            if kind == ROWS:
                wait_dispatched(b)
            elif kind == MIXER:
                mixer_group()
            gather.first()
            if kind == ROWS and b == 0:
                wait_weights()
                prepare_combine()
            elif kind == ROWS and b == 1:
                prepare_down()
        elif step < END:
            gather.step(step)
        else:
            gather.finish()
            if kind == ROWS:
                hidden(b)
            elif kind == HIDDEN:
                expert_result(b)
            else:
                mixed_result()

    others = (N_EP - 1) * CAP
    arrived(ret.at[pl.ds(0, others)], ret_r.at[0])
    results = ret[...]
    tokens_o[...] = (nn(combine[0], results) + nn(combine[1], results)).astype(BF16)

    for gather in gathers.values():
        gather.all_sent()
    for b in range(BATCHES):
        left(send_b.at[pl.ds(0, remote_rows(b)), pl.ds(0, 128 * COPIES[b])], disp_s.at[0])
    left(ret.at[pl.ds(0, others)], ret_s.at[0])


def per_device(
    mixer_input, mixer_gain, outer_weight, inner_weight, value_weight, conv_kernel, group_gain,
    mixer_out_weight, expert_input, expert_gain, routes, route_weight, expert_gate, expert_up,
    expert_down,
):
    phases = 2 * BATCHES + 1
    vmem = pltpu.VMEM
    dma = pltpu.SemaphoreType.DMA
    return pl.pallas_call(
        kernel,
        name="mixer_and_experts",
        out_shape=(
            jax.ShapeDtypeStruct((128, 128), BF16),
            jax.ShapeDtypeStruct((256, 128), BF16),
        ),
        in_specs=[pl.BlockSpec(memory_space=pl.ANY)] * 15,
        out_specs=(pl.BlockSpec(memory_space=vmem), pl.BlockSpec(memory_space=vmem)),
        scratch_shapes=[
            vmem((128, 2048), BF16),
            vmem((1, 2048), F32),
            vmem((192, 2048), BF16),
            vmem((3, 64), BF16),
            vmem((1, 64), F32),
            vmem((1024, 128), BF16),
            vmem((256, 2048), BF16),
            vmem((1, 2048), F32),
            vmem((2, 256), jnp.int32),
            vmem((2, 256), F32),
            vmem((448, 2048), BF16),
            vmem((3584, 128), BF16),
            vmem((1024, 256), BF16),
            vmem((N_EP, 256), F32),
            vmem((N_EP, 256), F32),
            vmem((2, 256, 1024), BF16),
            vmem((1024, 256), BF16),
            vmem((1024, 256), BF16),
            vmem((BATCHES, 256, 2048), BF16),
            vmem((BATCHES, 3584, 256), BF16),
            vmem((BATCHES, 256, 128), BF16),
            vmem((1024, 128), BF16),
            vmem((128, 3584), BF16),
            vmem((128, 1024), BF16),
            vmem((1024, 128), BF16),
            vmem((64, 128), F32),
            vmem((64, 128), F32),
            vmem((64, 128), F32),
            dma((15,)),
            dma((1,)),
            dma((BATCHES,)),
            dma((1,)),
            dma((1,)),
            dma((phases,)),
            dma((phases, 8)),
            dma((phases,)),
            dma((2,)),
        ],
        compiler_params=pltpu.CompilerParams(
            collective_id=0, has_side_effects=True, vmem_limit_bytes=56 * 1024 * 1024
        ),
    )(
        mixer_input, mixer_gain.reshape(1, -1), outer_weight.T, inner_weight.T, value_weight.T,
        conv_kernel, group_gain.reshape(1, -1), mixer_out_weight, expert_input,
        expert_gain.reshape(1, -1), routes.T, route_weight.T, expert_gate[0].T, expert_up[0].T,
        expert_down[0],
    )


def solution(mesh):
    placed = (
        P("ep", None), P(), P(None, "tp"), P(None, "tp"), P(None, "tp"), P(None, "tp"), P("tp"),
        P(None, "tp"), P("ep", None), P(), P("ep", None), P("ep", None), P("ep", None, "tp"),
        P("ep", None, "tp"), P("ep", None, "tp"),
    )
    return jax.shard_map(
        per_device,
        mesh=mesh,
        in_specs=placed,
        out_specs=(P("ep", "tp"), P("ep", "tp")),
        check_vma=False,
    )
```

```python
import functools

import jax
import jax.numpy as jnp
from jax import lax
from jax.experimental import pallas as pl
from jax.experimental.pallas import tpu as pltpu
from jax.sharding import PartitionSpec as P

EPS = 1e-06
MESH = pl.DeviceIdType.MESH
F32 = jnp.float32
BF16 = jnp.bfloat16
NZ, NX = 8, 4
N_EP = NZ * NX
N_Y = 8
N_TP = 2 * N_Y
BATCHES = 4
EARLY = 2
ROWS, HIDDEN, MIXER = "x", "h", "m"
ACROSS, END = 5, 9
ORDER = (
    (ROWS, 0, 0), (ROWS, 0, 5), (ROWS, 1, 0), (ROWS, 0, 1), (ROWS, 1, 1), (ROWS, 0, 2),
    (ROWS, 2, 0), (ROWS, 1, 2), (ROWS, 3, 0), (ROWS, 1, 3), (ROWS, 2, 1), (ROWS, 1, END),
    (ROWS, 0, 3), (ROWS, 3, 1), (ROWS, 2, 2), (HIDDEN, 1, 0), (ROWS, 0, END), (HIDDEN, 0, 0),
    (ROWS, 3, 2), (ROWS, 2, 3), (ROWS, 2, END), (ROWS, 3, 3), (HIDDEN, 2, 0), (ROWS, 3, END),
    (HIDDEN, 3, 0), (HIDDEN, 1, 1), (HIDDEN, 2, 1), (HIDDEN, 3, 1), (MIXER, 0, 0), (HIDDEN, 1, 2),
    (HIDDEN, 3, 2), (HIDDEN, 0, 1), (HIDDEN, 2, 2), (HIDDEN, 3, 3), (HIDDEN, 0, 2), (MIXER, 0, 1),
    (HIDDEN, 2, 3), (HIDDEN, 1, 3), (HIDDEN, 3, 4), (HIDDEN, 0, 3), (HIDDEN, 3, END), (HIDDEN, 2, 4),
    (MIXER, 0, 2), (HIDDEN, 1, 4), (HIDDEN, 2, END), (HIDDEN, 0, 4), (HIDDEN, 1, END), (MIXER, 0, 3),
    (HIDDEN, 0, END), (MIXER, 0, 4), (MIXER, 0, END),
)
CAP = 32
PER = N_EP // BATCHES


GROUPS = (
    ((0, 2), (1, 1), (7, 3), (1, 0), (7, 0), (0, 1), (0, 3), (0, 0)),
    ((2, 0), (6, 0), (1, 3), (7, 1), (2, 1), (6, 3), (1, 2), (7, 2)),
    ((2, 2), (6, 2), (3, 0), (5, 0), (2, 3), (6, 1), (3, 1), (5, 3)),
    ((4, 0), (5, 1), (3, 3), (4, 1), (5, 2), (3, 2), (4, 3), (4, 2)),
)
COPIES = (2, 2, 2, 2)


def nt(a, b):
    return lax.dot_general(a, b, (((1,), (1,)), ((), ())), preferred_element_type=F32)


def nn(a, b):
    return lax.dot_general(a, b, (((1,), (0,)), ((), ())), preferred_element_type=F32)


def eye(n):
    return (
        lax.broadcasted_iota(jnp.int32, (n, n), 0) == lax.broadcasted_iota(jnp.int32, (n, n), 1)
    )


def column(row, mask):
    return jnp.sum(jnp.where(mask, row, 0.0), axis=1, keepdims=True)


def kernel(
    mixin_h, mgain_h, outer_h, inner_h, value_h, conv_h, ggain_h, mout_h,
    expin_h, egain_h, routes_h, rweight_h, gate_h, up_h, down_h,
    mixed_o, tokens_o,
    mixin, mgain, mproj, conv, ggain, mout,
    expin, egain, routes, rweight, gateup, down,
    onehot, pos32, wsel32, combine, wide_t, send_b, xs, hs, y_b, ret,
    down_t, mout_t, grouped, prod_s, halo, outer_s,
    load_sem, disp_s, disp_r, ret_s, ret_r, sent, ring_r, part_r, halo_sem,
):
    ep = lax.axis_index("ep")
    tp = lax.axis_index("tp")
    z, x = ep // NX, lax.rem(ep, NX)
    core = lax.rem(tp, 2)
    mate = tp + 1 - 2 * core
    y_of = tp // 2

    def ep_at(dz, dx):
        return lax.rem(z + dz + NZ, NZ) * NX + lax.rem(x + dx + NX, NX)

    def ring_tp(d):
        return lax.rem(tp + 2 * d + N_TP, N_TP)

    across = ring_tp(N_Y // 2)
    low = lax.rem(tp, N_Y)

    def features(j):
        return pl.ds(pl.multiple_of(j * 128, 128), 128)

    def place(j):
        return features(2 * lax.rem(j, N_Y) + j // N_Y)

    sources = dict(
        routes=(routes_h, routes),
        expin=(expin_h, expin),
        egain=(egain_h, egain),
        mixin=(mixin_h, mixin),
        mgain=(mgain_h, mgain),
        outer=(outer_h, mproj.at[pl.ds(0, 64)]),
        inner=(inner_h, mproj.at[pl.ds(64, 64)]),
        value=(value_h, mproj.at[pl.ds(128, 64)]),
        conv=(conv_h, conv),
        ggain=(ggain_h, ggain),
        rweight=(rweight_h, rweight),
        down=(down_h, down),
        mout=(mout_h, mout),
    )
    loads = {
        name: pltpu.make_async_copy(src, dst, load_sem.at[i])
        for i, (name, (src, dst)) in enumerate(sources.items())
    }
    urgent = ("routes", "expin", "egain")
    for name in urgent:
        loads[name].start()

    barrier = pltpu.get_barrier_semaphore()
    for dz, dx in (o for group in GROUPS for o in group if o != (0, 0)):
        pl.semaphore_signal(barrier, inc=1, device_id=(ep_at(dz, dx), tp), device_id_type=MESH)
    for other in (ring_tp(1), ring_tp(-1), mate):
        pl.semaphore_signal(barrier, inc=1, device_id=(ep, other), device_id_type=MESH)

    loads["routes"].wait()
    first, second = routes[0:1, :], routes[1:2, :]
    expert = lax.broadcasted_iota(jnp.int32, (N_EP, 256), 0)
    is_first = first == expert
    named = is_first | (second == expert)
    before = lax.broadcasted_iota(jnp.int32, (256, 256), 0) < lax.broadcasted_iota(
        jnp.int32, (256, 256), 1
    )
    rank = nn(jnp.where(named, 1.0, 0.0).astype(BF16), jnp.where(before, 1.0, 0.0).astype(BF16))
    pos32[...] = jnp.where(named, rank, -1.0)
    slot = lax.broadcasted_iota(jnp.int32, (CAP, 256), 0).astype(F32)
    for e in range(N_EP):
        onehot[e * CAP : (e + 1) * CAP, :] = jnp.where(slot == pos32[e : e + 1, :], 1.0, 0.0).astype(
            BF16
        )

    loads["expin"].wait()
    loads["egain"].wait()
    for name in loads:
        if name not in urgent:
            loads[name].start()
    for part, weight in enumerate((gate_h, up_h)):
        for j in range(N_TP):
            pltpu.make_async_copy(
                weight.at[:, pl.ds(j * 128, 128)],
                gateup.at[pl.ds(part * 224, 224), pl.ds((2 * (j % N_Y) + j // N_Y) * 128, 128)],
                load_sem.at[len(loads)],
            ).start()
    rows = expin[...].astype(F32)
    scale = lax.rsqrt(jnp.mean(rows * rows, axis=-1, keepdims=True) + EPS)
    normed_b = jnp.concatenate(
        [
            (expin[:, part].astype(F32) * scale * egain[:, part]).astype(BF16)
            for part in (features(low), features(low + N_Y))
        ],
        axis=1,
    )
    send_b[...] = nn(onehot[...], normed_b).astype(BF16)

    pl.semaphore_wait(barrier, N_EP - 1 + 3)

    def dispatch_parts(b, i, target, second):
        rows = pl.ds(pl.multiple_of(target * CAP, CAP), CAP)
        if COPIES[b] == 2 and b > 0:
            to = pl.ds(pl.multiple_of(low * 256, 256), 256)
            return send_b.at[rows], xs.at[b, pl.ds(i * CAP, CAP), to]
        half, chunk = (1 - tp // N_Y, across) if second else (tp // N_Y, tp)
        return send_b.at[rows, features(half)], xs.at[b, pl.ds(i * CAP, CAP), place(chunk)]

    def dispatch_batch(b, second=False):
        for i, (dz, dx) in enumerate(GROUPS[b]):
            target = ep_at(-dz, -dx)
            src, dst = dispatch_parts(b, i, target, second)
            if (dz, dx) == (0, 0):
                dst[...] = src[...]
            else:
                pltpu.make_async_remote_copy(
                    src_ref=src, dst_ref=dst, send_sem=disp_s.at[0],
                    recv_sem=disp_r.at[BATCHES if second else b],
                    device_id=(target, tp), device_id_type=MESH,
                ).start()

    dispatch_batch(0)
    dispatch_batch(0, second=True)
    for b in range(1, EARLY):
        dispatch_batch(b)

    for name in ("mixin", "mgain", "outer", "inner", "value"):
        loads[name].wait()
    rows_a = mixin[...].astype(F32)
    scale_a = lax.rsqrt(jnp.mean(rows_a * rows_a, axis=-1, keepdims=True) + EPS)
    normed_a = (rows_a * scale_a * mgain[...]).astype(BF16)
    projected = nt(mproj[...], normed_a).astype(BF16).astype(F32)
    outer_s[...] = projected[0:64]
    prod_s[...] = projected[64:128] * projected[128:192]
    next_ep = lax.rem(ep + 1, N_EP)
    halo_copy = pltpu.make_async_remote_copy(
        src_ref=prod_s,
        dst_ref=halo,
        send_sem=halo_sem.at[0],
        recv_sem=halo_sem.at[1],
        device_id=(next_ep, tp),
        device_id_type=MESH,
    )
    halo_copy.start()
    for b in range(EARLY, BATCHES):
        dispatch_batch(b)

    def mixer_group():
        halo_copy.wait()
        for name in ("conv", "ggain"):
            loads[name].wait()
        product = prod_s[...]
        behind = jnp.where(ep > 0, halo[...], 0.0)
        lane = lax.broadcasted_iota(jnp.int32, (64, 128), 1)
        one = jnp.where(lane < 1, pltpu.roll(behind, 1, 1), pltpu.roll(product, 1, 1))
        two = jnp.where(lane < 2, pltpu.roll(behind, 2, 1), pltpu.roll(product, 2, 1))
        mask = eye(64)
        taps = [column(conv[i : i + 1, :].astype(F32), mask) for i in range(3)]
        conv_sum = taps[0] * two + taps[1] * one + taps[2] * product
        gated = outer_s[...] * conv_sum
        norm = lax.rsqrt(jnp.mean(gated * gated, axis=0, keepdims=True) + EPS)
        own = pl.ds(pl.multiple_of(tp * 64, 64), 64)
        grouped[own, :] = (gated * norm * column(ggain[...], mask)).astype(BF16)

    def prepare_combine():
        loads["rweight"].wait()
        weight = jnp.where(is_first, rweight[0:1, :], rweight[1:2, :])
        high = weight.astype(BF16).astype(F32)
        identity = jnp.where(eye(256), 1.0, 0.0).astype(BF16)
        for part, value in enumerate((high, weight - high)):
            wsel32[...] = value
            for e in range(N_EP):
                wide_t[e * CAP : (e + 1) * CAP, :] = jnp.where(
                    slot == pos32[e : e + 1, :], wsel32[e : e + 1, :], 0.0
                ).astype(BF16)
            combine[part] = nt(identity, wide_t[...]).astype(BF16)

    def prepare_down():
        loads["down"].wait()
        identity = jnp.where(eye(128), 1.0, 0.0).astype(BF16)
        down_t[...] = nt(identity, down[...]).astype(BF16)
        loads["mout"].wait()
        mout_t[...] = nt(identity, mout[...]).astype(BF16)

    def piece_of(kind, b):
        if kind == ROWS:
            return lambda j, h=0, n=1: xs.at[b, pl.ds(h * 128, 256 // n), place(j)]
        if kind == HIDDEN:
            return lambda j, h=0, n=1: hs.at[b, pl.ds(pl.multiple_of(j * 224 + h * 112, 16), 224 // n)]
        return lambda j, h=0, n=1: grouped.at[pl.ds(pl.multiple_of(j * 64 + h * 32, 32), 64 // n)]

    def part_of(kind, b):
        if kind == ROWS:
            return lambda n: xs.at[b, :, pl.ds(0, n * 128)]
        if kind == HIDDEN:
            return lambda n: hs.at[b, pl.ds(0, n * 224)]
        return lambda n: grouped.at[pl.ds(0, n * 64)]

    def arrived(ref, sem):
        pltpu.make_async_remote_copy(
            src_ref=ref, dst_ref=ref, send_sem=disp_s.at[0], recv_sem=sem,
            device_id=(ep, mate), device_id_type=MESH,
        ).wait_recv()

    def left(ref, sem):
        pltpu.make_async_remote_copy(
            src_ref=ref, dst_ref=ref, send_sem=sem, recv_sem=disp_r.at[0],
            device_id=(ep, mate), device_id_type=MESH,
        ).wait_send()

    def remote_rows(b):
        return CAP * sum(o != (0, 0) for o in GROUPS[b])

    def send(src, dst, send_sem, recv_sem, to):
        copy = pltpu.make_async_remote_copy(
            src_ref=src, dst_ref=dst, send_sem=send_sem, recv_sem=recv_sem,
            device_id=(ep, to), device_id_type=MESH,
        )
        copy.start()

    class Gather:
        def __init__(self, number, kind, b):
            self.n, self.piece, self.part = number, piece_of(kind, b), part_of(kind, b)

        def received(self, way, k):
            return ring_r.at[self.n, (k if way == 1 else 4 + k) - 1]

        def on_ring(self, ref, way, k):
            send(ref, ref, sent.at[self.n], self.received(way, k), ring_tp(way))

        def to_mate(self, ref):
            send(ref, ref, sent.at[self.n], part_r.at[self.n], mate)

        def first(self):
            ref = self.piece(tp)
            self.to_mate(ref)
            self.on_ring(ref, 1, 1)
            self.on_ring(ref, -1, 1)

        def step(self, k):
            for way, h in ((1, 0), (-1, 1)):
                j = ring_tp(-way * k)
                ref = self.piece(j) if k < 4 else self.piece(j, h, 2)
                arrived(ref, self.received(way, k))
                self.to_mate(ref)
                if k < 4:
                    self.on_ring(ref if k < 3 else self.piece(j, h, 2), way, k + 1)

        def finish(self):
            arrived(self.part(N_Y), part_r.at[self.n])

        def all_sent(self):
            left(self.part(N_TP - 1), sent.at[self.n])

    class PairGather(Gather):
        def first(self):
            super().first()
            if self.n > 0:
                self.second()

        def second(self):
            ref = self.piece(across)
            self.to_mate(ref)
            self.on_ring(ref, 1, 2)
            self.on_ring(ref, -1, 2)

        def step(self, k):
            for way in (1, -1):
                ref = self.piece(ring_tp((-way, 3 * way, -2 * way)[k - 1]))
                arrived(ref, self.received(way, k))
                self.to_mate(ref)
                if k == 1:
                    self.on_ring(ref, way, 3)

        def all_sent(self):
            left(self.part(N_TP - 2), sent.at[self.n])

    def wait_dispatched(b):
        width = 128 if b == 0 else 128 * COPIES[b]
        arrived(xs.at[b, pl.ds(0, remote_rows(b)), pl.ds(0, width)], disp_r.at[b])

    def hidden(b):
        both = nt(gateup[...], xs[b])
        gate, up = both[0:224], both[224:448]
        own = pl.ds(pl.multiple_of(tp * 224, 224), 224)
        hs[b, own, :] = (gate / (1.0 + jnp.exp(-gate)) * up).astype(BF16)

    def give_back(b, i):
        dz, dx = GROUPS[b][i]
        target = ep_at(dz, dx)
        return pltpu.make_async_remote_copy(
            src_ref=y_b.at[b, pl.ds(i * CAP, CAP)],
            dst_ref=ret.at[pl.ds(pl.multiple_of(ep * CAP, CAP), CAP)],
            send_sem=ret_s.at[0],
            recv_sem=ret_r.at[0],
            device_id=(target, tp),
            device_id_type=MESH,
        )

    def expert_result(b):
        out_t = nn(down_t[...], hs[b]).astype(BF16)
        identity = jnp.where(eye(256), 1.0, 0.0).astype(BF16)
        y_b[b] = nt(identity, out_t).astype(BF16)
        for i, o in enumerate(GROUPS[b]):
            if o != (0, 0):
                give_back(b, i).start()
            else:
                ret[pl.ds(pl.multiple_of(ep * CAP, CAP), CAP), :] = y_b[b, i * CAP : (i + 1) * CAP, :]

    def mixed_result():
        mixed_t = nn(mout_t[...], grouped[...]).astype(BF16)
        identity = jnp.where(eye(128), 1.0, 0.0).astype(BF16)
        mixed_o[...] = nt(identity, mixed_t).astype(BF16)

    def wait_weights():
        pltpu.make_async_copy(gateup, gateup, load_sem.at[len(loads)]).wait()

    gathers = {(MIXER, 0): Gather(2 * BATCHES, MIXER, 0)}
    for b in range(BATCHES):
        gathers[ROWS, b] = (PairGather if COPIES[b] == 2 else Gather)(b, ROWS, b)
        gathers[HIDDEN, b] = Gather(BATCHES + b, HIDDEN, b)

    for kind, b, step in ORDER:
        gather = gathers[kind, b]
        if step == 0:
            if kind == ROWS:
                wait_dispatched(b)
            elif kind == MIXER:
                mixer_group()
            gather.first()
            if kind == ROWS and b == 0:
                wait_weights()
                prepare_combine()
            elif kind == ROWS and b == 1:
                prepare_down()
        elif step == ACROSS:
            arrived(xs.at[0, pl.ds(0, remote_rows(0)), pl.ds(0, 128)], disp_r.at[BATCHES])
            gather.second()
        elif step < END:
            gather.step(step)
        else:
            gather.finish()
            if kind == ROWS:
                hidden(b)
            elif kind == HIDDEN:
                expert_result(b)
            else:
                mixed_result()

    others = (N_EP - 1) * CAP
    arrived(ret.at[pl.ds(0, others)], ret_r.at[0])
    results = ret[...]
    tokens_o[...] = (nn(combine[0], results) + nn(combine[1], results)).astype(BF16)

    for gather in gathers.values():
        gather.all_sent()
    for b in range(BATCHES):
        left(send_b.at[pl.ds(0, remote_rows(b)), pl.ds(0, 128 * COPIES[b])], disp_s.at[0])
    left(ret.at[pl.ds(0, others)], ret_s.at[0])


def per_device(
    mixer_input, mixer_gain, outer_weight, inner_weight, value_weight, conv_kernel, group_gain,
    mixer_out_weight, expert_input, expert_gain, routes, route_weight, expert_gate, expert_up,
    expert_down,
):
    phases = 2 * BATCHES + 1
    vmem = pltpu.VMEM
    dma = pltpu.SemaphoreType.DMA
    return pl.pallas_call(
        kernel,
        name="mixer_and_experts",
        out_shape=(
            jax.ShapeDtypeStruct((128, 128), BF16),
            jax.ShapeDtypeStruct((256, 128), BF16),
        ),
        in_specs=[pl.BlockSpec(memory_space=pl.ANY)] * 15,
        out_specs=(pl.BlockSpec(memory_space=vmem), pl.BlockSpec(memory_space=vmem)),
        scratch_shapes=[
            vmem((128, 2048), BF16),
            vmem((1, 2048), F32),
            vmem((192, 2048), BF16),
            vmem((3, 64), BF16),
            vmem((1, 64), F32),
            vmem((1024, 128), BF16),
            vmem((256, 2048), BF16),
            vmem((1, 2048), F32),
            vmem((2, 256), jnp.int32),
            vmem((2, 256), F32),
            vmem((448, 2048), BF16),
            vmem((3584, 128), BF16),
            vmem((1024, 256), BF16),
            vmem((N_EP, 256), F32),
            vmem((N_EP, 256), F32),
            vmem((2, 256, 1024), BF16),
            vmem((1024, 256), BF16),
            vmem((1024, 256), BF16),
            vmem((BATCHES, 256, 2048), BF16),
            vmem((BATCHES, 3584, 256), BF16),
            vmem((BATCHES, 256, 128), BF16),
            vmem((1024, 128), BF16),
            vmem((128, 3584), BF16),
            vmem((128, 1024), BF16),
            vmem((1024, 128), BF16),
            vmem((64, 128), F32),
            vmem((64, 128), F32),
            vmem((64, 128), F32),
            dma((15,)),
            dma((1,)),
            dma((BATCHES + 1,)),
            dma((1,)),
            dma((1,)),
            dma((phases,)),
            dma((phases, 8)),
            dma((phases,)),
            dma((2,)),
        ],
        compiler_params=pltpu.CompilerParams(
            collective_id=0, has_side_effects=True, vmem_limit_bytes=56 * 1024 * 1024
        ),
    )(
        mixer_input, mixer_gain.reshape(1, -1), outer_weight.T, inner_weight.T, value_weight.T,
        conv_kernel, group_gain.reshape(1, -1), mixer_out_weight, expert_input,
        expert_gain.reshape(1, -1), routes.T, route_weight.T, expert_gate[0].T, expert_up[0].T,
        expert_down[0],
    )


def solution(mesh):
    placed = (
        P("ep", None), P(), P(None, "tp"), P(None, "tp"), P(None, "tp"), P(None, "tp"), P("tp"),
        P(None, "tp"), P("ep", None), P(), P("ep", None), P("ep", None), P("ep", None, "tp"),
        P("ep", None, "tp"), P("ep", None, "tp"),
    )
    return jax.shard_map(
        per_device,
        mesh=mesh,
        in_specs=placed,
        out_specs=(P("ep", "tp"), P("ep", "tp")),
        check_vma=False,
    )
```
